32 devices in a mesh: ep: 8 (over z, x), tp: 4 (over y, core).
Axes of the slice: x: 2, y: 2, z: 4, core: 2. Of those that a mesh axis runs over, the one named last changes fastest.
Arguments:
- queries: bfloat16 [4096, 8, 96], P('ep', 'tp'), may hold values from -240 to 240
- kv_latent: bfloat16 [4096, 128], P(('ep', 'tp')), may hold values from -6 to 6
- rope_key: bfloat16 [4096, 32], P(('ep', 'tp')), may hold values from -6 to 6
- kv_gain: float32 [128], replicated, may hold values from 0.1 to 1.9
- kv_up: bfloat16 [128, 8, 128], P(None, 'tp'), may hold values from -0.5 to 0.5
- mix_out: bfloat16 [8, 64, 2048], P('tp'), may hold values from -0.25 to 0.25
- moe_in: bfloat16 [2048, 2048], P('ep', 'tp'), may hold values from -6 to 6
- moe_gain: float32 [2048], replicated, may hold values from 0.1 to 1.9
- routes: int32 [2048, 2], P('ep'), may hold values from 0 to 7, all different within a row; in each aligned block of 256 rows (0 to 255, 256 to 511, ...) at most 68 rows name the same one
- route_weights: float32 [2048, 2], P('ep'), may hold values from 0.1 to 1
- gate_w: bfloat16 [8, 2048, 3584], P('ep', None, 'tp'), may hold values from -0.125 to 0.125
- up_w: bfloat16 [8, 2048, 3584], P('ep', None, 'tp'), may hold values from -0.125 to 0.125
- down_w: bfloat16 [8, 3584, 2048], P('ep', 'tp'), may hold values from -0.09375 to 0.09375
Outputs:
- mixed: bfloat16 [4096, 2048], P(('ep', 'tp'))
- moe_out: bfloat16 [2048, 2048], P('ep', 'tp')
The draws below stay inside these ranges and needn't reach their ends.
Inputs may be any that keep to these rules, and one draw needn't show every extreme that they name: `routes`: among the rows of one index of ep, no expert is named by more than 68 entries, a bound that some block reaches; a row names 2 different experts.
All inputs are finite; a program needn't handle non-finite values.
Results may differ from the reference program's by a relative error of at most 0.025.
Values may be sent and summed in bfloat16 or wider, within the bound.
A program may use at most 128 MiB of HBM per device.

```python
import math
import jax
import jax.numpy as jnp
import numpy as np
from jax import lax

D = 2048
HEADS = 8
NOPE = 64
ROPE = 32
VDIM = 64
KVLAT = 128
FFE = 3584
TOP = 2
EXPERTS = 8
TOKENS_A = 4096
SEQ_LEN = 4096
ROWS_E = 256
TOKENS_E = 2048
CAP = 68
N_EP = 8
N_TP = 4


def draw_queries(key, part):
    base_key = jax.random.fold_in(jax.random.fold_in(key, 11), 0)
    draw_shape = (TOKENS_A, HEADS, NOPE + ROPE)
    normal_part = jnp.clip(jax.random.normal(base_key, draw_shape, jnp.float32), -4.0, 4.0)
    return normal_part.astype(jnp.bfloat16)


def levels(stream_key, shape, cuts, low, high):
    def one(dim, shards_of):
        steps = jax.random.uniform(jax.random.fold_in(jax.random.fold_in(stream_key, 6), dim), (shards_of,), jnp.float32, low / len(cuts), high / len(cuts))
        return jnp.repeat(jnp.exp(steps), shape[dim] // shards_of).reshape((-1,) + (1,) * (len(shape) - dim - 1))

    level = one(*cuts[0])
    for cut in cuts[1:]:
        level = level * one(*cut)
    return level


def assign_block(key, own, number, rows, amount, top, reach, slope):
    ranking = jax.random.permutation(key, amount)
    crowded, ordinary = load_shares(amount, rows * top, reach, slope, True), load_shares(amount, rows * top, reach, slope, False)
    places = jnp.arange(amount)

    def named(tallies, offset_by):
        used = int((tallies > 0).sum())
        fixed = max(1, used // 4)
        moved = fixed + (places - fixed + offset_by * (used - fixed)) % max(1, amount - fixed)
        return jnp.zeros((amount,), jnp.int32).at[ranking[jnp.where(places < fixed, places, moved)]].set(jnp.asarray(tallies, jnp.int32))

    tallies = jnp.where(number % 4 == 0, named(crowded, number // 4), named(ordinary, number - number // 4 - 1))
    mixed = jax.random.permutation(jax.random.fold_in(own, 3), amount)
    source_of, receiver = mixed[0:amount // 2 * 2:2], mixed[1:amount // 2 * 2:2]
    room = jnp.minimum(tallies[source_of] - 1, reach - tallies[receiver]) // 2
    room = jnp.where((source_of == ranking[0]) | (receiver == ranking[0]) | (tallies[receiver] == 0), 0, jnp.maximum(room, 0))
    moved = jax.random.randint(jax.random.fold_in(own, 4), (amount // 2,), 0, 1 << 20) % (room + 1)
    tallies = tallies.at[source_of].add(-moved).at[receiver].add(moved)
    items = jnp.searchsorted(jnp.cumsum(tallies), jnp.arange(rows * top), side="right").astype(jnp.int32)
    listing = items.reshape(top, rows).T
    listing = listing[jax.random.permutation(jax.random.fold_in(own, 1), rows)]
    offset_by = jax.random.randint(jax.random.fold_in(own, 2), (rows, 1), 0, top)
    return jnp.take_along_axis(listing, (jnp.arange(top)[None, :] + offset_by) % top, axis=1)


def load_shares(count, total, limit, lean, full):
    weights = [(1 << 20) // math.isqrt(grade ** lean) + 1 for grade in range(1, count + 1)]
    largest = limit if full else min(limit, max(-(-total // count), total * weights[0] // sum(weights)))
    least = 1 if total - largest >= count - 1 else 0
    given, rest = [largest] + [least] * (count - 1), total - largest - least * (count - 1)
    while rest > 0:
        candidates = [i for i in range(1, count) if given[i] < largest] or [i for i in range(1, count) if given[i] < limit]
        mass, remaining = sum([weights[i] for i in candidates]), rest
        for i in candidates:
            extra = min(limit - given[i], max(1, remaining * weights[i] // mass), rest)
            given[i] = given[i] + extra
            rest = rest - extra
    return np.array(given)


def scatter_about(own_key, dims, deviation, most, pieces=(), kind=jnp.bfloat16):
    array = deviation * jax.random.normal(own_key, dims, jnp.float32)
    if pieces:
        array = array * levels(own_key, dims, pieces, -0.22, 0.18)
    return jnp.clip(array, -most, most).astype(kind)


def setup_inputs(seed: int = 0) -> dict:
    seeds = jax.random.split(jax.random.key(seed), 14)
    queries = draw_queries(jax.random.fold_in(seeds[13], 71), 0)
    kv_latent = scatter_about(seeds[1], (TOKENS_A, KVLAT), 1.0, 6.0, ((0, 32),))
    rope_key = scatter_about(seeds[2], (TOKENS_A, ROPE), 1.0, 6.0, ((0, 32),))
    kv_gain = jnp.clip(1.0 + 0.18 * jax.random.normal(seeds[3], (KVLAT,), jnp.float32), 0.1, 1.9)
    kv_up = scatter_about(seeds[4], (KVLAT, HEADS, NOPE + VDIM), KVLAT ** -0.5, 0.5, ((1, 4),))
    mix_out = scatter_about(seeds[5], (HEADS, VDIM, D), (HEADS * VDIM) ** -0.5, 0.25, ((0, 4),))
    moe_in = scatter_about(seeds[6], (TOKENS_E, D), 1.0, 6.0, ((0, 8), (1, 4)))
    moe_gain = jnp.clip(1.0 + 0.18 * jax.random.normal(seeds[7], (D,), jnp.float32), 0.1, 1.9)
    routes_keys = jax.random.split(jax.random.fold_in(seeds[8], 1), TOKENS_E // ROWS_E)
    routes_turns = jax.random.permutation(jax.random.fold_in(seeds[8], 3), TOKENS_E // ROWS_E)
    routes = jax.vmap(lambda own, number: assign_block(jax.random.fold_in(seeds[8], 2), own, number, ROWS_E, EXPERTS, TOP, CAP, 1))(routes_keys, routes_turns).reshape((TOKENS_E, TOP))
    route_weights = jnp.clip(0.1 + 0.9 * jax.random.uniform(seeds[9], (TOKENS_E, TOP), jnp.float32) ** levels(seeds[9], (TOKENS_E, TOP), ((0, 8),), -0.2, 0.2), 0.1, 1.0)
    gate_w = scatter_about(seeds[10], (EXPERTS, D, FFE), D ** -0.5, 0.125, ((0, 8), (2, 4)))
    up_w = scatter_about(seeds[11], (EXPERTS, D, FFE), D ** -0.5, 0.125, ((0, 8), (2, 4)))
    down_w = scatter_about(seeds[12], (EXPERTS, FFE, D), FFE ** -0.5, 0.09375, ((0, 8), (1, 4)))
    return dict(queries=queries, kv_latent=kv_latent, rope_key=rope_key, kv_gain=kv_gain, kv_up=kv_up, mix_out=mix_out, moe_in=moe_in, moe_gain=moe_gain, routes=routes, route_weights=route_weights, gate_w=gate_w, up_w=up_w, down_w=down_w)


eps = 1e-06
rope_base = 10000.0
neg_big = -1e+30

def rotate(values, positions):
    half_dim = values.shape[-1] // 2
    inv_freq = rope_base ** (-jnp.arange(half_dim, dtype=jnp.float32) * 2.0 / values.shape[-1])
    angles = positions.astype(jnp.float32)[:, None] * inv_freq[None, :]
    angles = angles.reshape((angles.shape[0],) + (1,) * (values.ndim - 2) + (half_dim,))
    cosine = jnp.cos(angles)
    sine_part = jnp.sin(angles)
    first_half = values[..., :half_dim].astype(jnp.float32)
    second_half = values[..., half_dim:].astype(jnp.float32)
    return jnp.concatenate([first_half * cosine - second_half * sine_part, second_half * cosine + first_half * sine_part], axis=-1)

def slot_table(block_routes):
    flat_routes = block_routes.reshape(-1)
    onehot = (flat_routes[:, None] == jnp.arange(EXPERTS, dtype=jnp.int32)[None, :]).astype(jnp.int32)
    slot_rank = lax.optimization_barrier(jnp.sum((jnp.cumsum(onehot, axis=0) - onehot) * onehot, axis=1))
    slot_dest = flat_routes * CAP + slot_rank
    slot_owner = jnp.full((EXPERTS * CAP,), -1, jnp.int32).at[slot_dest].set(jnp.arange(flat_routes.shape[0], dtype=jnp.int32))
    return (slot_dest, slot_owner)

def reference(queries, kv_latent, rope_key, kv_gain, kv_up, mix_out, moe_in, moe_gain, routes, route_weights, gate_w, up_w, down_w):
    total_rows = queries.shape[0]
    token_index = jnp.arange(total_rows, dtype=jnp.int32)
    positions = token_index % SEQ_LEN
    query_nope = queries[..., :NOPE]
    query_rot = rotate(queries[..., NOPE:], positions).astype(jnp.bfloat16)
    latent_f = kv_latent.astype(jnp.float32)
    normed = (latent_f * lax.rsqrt(lax.optimization_barrier(jnp.mean(latent_f * latent_f, axis=-1, keepdims=True)) + eps) * kv_gain).astype(jnp.bfloat16)
    head_proj = jnp.einsum('nr,rhd->nhd', normed.astype(jnp.float32), kv_up.astype(jnp.float32)).astype(jnp.bfloat16)
    key_nope = head_proj[..., :NOPE]
    values = head_proj[..., NOPE:]
    key_rot = rotate(rope_key, positions).astype(jnp.bfloat16)
    query_block = min(512, SEQ_LEN)
    score_scale = 1.0 / math.sqrt(NOPE + ROPE)

    def attend_block(first_row):
        seq_start = first_row // SEQ_LEN * SEQ_LEN
        block_nope = lax.dynamic_slice_in_dim(query_nope, first_row, query_block, 0).astype(jnp.float32)
        block_rot = lax.dynamic_slice_in_dim(query_rot, first_row, query_block, 0).astype(jnp.float32)
        seq_nope = lax.dynamic_slice_in_dim(key_nope, seq_start, SEQ_LEN, 0).astype(jnp.float32)
        seq_rot = lax.dynamic_slice_in_dim(key_rot, seq_start, SEQ_LEN, 0).astype(jnp.float32)
        seq_values = lax.dynamic_slice_in_dim(values, seq_start, SEQ_LEN, 0).astype(jnp.float32)
        scores = (jnp.einsum('qhd,khd->qhk', block_nope, seq_nope) + jnp.einsum('qhd,kd->qhk', block_rot, seq_rot)) * score_scale
        query_ids = first_row + jnp.arange(query_block, dtype=jnp.int32)
        key_ids = seq_start + jnp.arange(SEQ_LEN, dtype=jnp.int32)
        allowed = (key_ids[None, :] <= query_ids[:, None])[:, None, :]
        scores = jnp.where(allowed, scores, neg_big)
        row_max = lax.optimization_barrier(jnp.max(scores, axis=-1, keepdims=True))
        probs = jnp.where(allowed, jnp.exp(scores - row_max), 0.0)
        denom = lax.optimization_barrier(jnp.sum(probs, axis=-1))
        weighted = jnp.einsum('qhk,khd->qhd', probs.astype(jnp.bfloat16).astype(jnp.float32), seq_values)
        return (weighted / denom[..., None]).astype(jnp.bfloat16)
    starts = jnp.arange(0, total_rows, query_block, dtype=jnp.int32)
    attn = lax.map(attend_block, starts).reshape(total_rows, HEADS, VDIM)
    group_heads = HEADS // N_TP
    mixed = jnp.zeros((total_rows, D), jnp.float32)
    for group in range(N_TP):
        part_sum = jnp.einsum('thv,hvd->td', attn[:, group * group_heads:(group + 1) * group_heads].astype(jnp.float32), mix_out[group * group_heads:(group + 1) * group_heads].astype(jnp.float32))
        rounded = lax.optimization_barrier(part_sum.astype(jnp.bfloat16))
        mixed = mixed + rounded.astype(jnp.float32)
    mixed = mixed.astype(jnp.bfloat16)
    slot_dest, slot_owner = jax.vmap(slot_table)(routes.reshape(N_EP, ROWS_E, TOP))
    moe_f = moe_in.astype(jnp.float32)
    row_scale = lax.rsqrt(lax.optimization_barrier(jnp.mean(moe_f * moe_f, axis=-1)) + eps)
    scaled = (moe_f * moe_gain).astype(jnp.bfloat16)
    owner_by_expert = slot_owner.reshape(N_EP, EXPERTS, CAP).transpose(1, 0, 2)
    block_base = (jnp.arange(N_EP, dtype=jnp.int32) * ROWS_E)[:, None]
    quarter = FFE // N_TP

    def serve_expert(inputs):
        expert, slots = inputs
        is_valid = (slots >= 0).reshape(-1)
        token_row = (block_base + jnp.maximum(slots, 0) // TOP).reshape(-1)
        picked_rows = scaled[token_row].astype(jnp.float32)
        picked_scale = row_scale[token_row][:, None]
        gate = jnp.dot(picked_rows, gate_w[expert].astype(jnp.float32)) * picked_scale
        up_val = jnp.dot(picked_rows, up_w[expert].astype(jnp.float32)) * picked_scale
        hidden = (jax.nn.silu(gate) * up_val).astype(jnp.bfloat16)
        down_expert = down_w[expert]
        expert_sum = jnp.zeros((hidden.shape[0], D), jnp.float32)
        for group in range(N_TP):
            part_sum = jnp.dot(hidden[:, group * quarter:(group + 1) * quarter].astype(jnp.float32), down_expert[group * quarter:(group + 1) * quarter].astype(jnp.float32))
            rounded = lax.optimization_barrier(part_sum.astype(jnp.bfloat16))
            expert_sum = expert_sum + rounded.astype(jnp.float32)
        return jnp.where(is_valid[:, None], expert_sum, 0.0).astype(jnp.bfloat16)
    results = lax.map(serve_expert, (jnp.arange(EXPERTS, dtype=jnp.int32), owner_by_expert)).reshape(EXPERTS, N_EP, CAP, D)
    route_flat = routes.reshape(N_EP, ROWS_E * TOP)
    slot_pos = slot_dest - route_flat * CAP
    block_ids = jnp.broadcast_to(jnp.arange(N_EP, dtype=jnp.int32)[:, None], route_flat.shape)
    picked = results[route_flat, block_ids, slot_pos].astype(jnp.float32).reshape(TOKENS_E, TOP, D)
    moe_out = lax.optimization_barrier(jnp.sum(picked * route_weights[..., None], axis=1)).astype(jnp.bfloat16)
    return (mixed, moe_out)
```

```python
import functools
import math

import jax
import jax.numpy as jnp
from jax import lax
from jax.experimental import pallas as pl
from jax.experimental.pallas import tpu as pltpu
from jax.sharding import PartitionSpec as P

D = 2048
NOPE = 64
SEQS = 1


eps = 1e-06
rope_base = 10000.0
neg_big = -1e30


def rotate(values, positions):
    half_dim = values.shape[-1] // 2
    inv_freq = rope_base ** (-jnp.arange(half_dim, dtype=jnp.float32) * 2.0 / values.shape[-1])
    angles = positions.astype(jnp.float32)[:, None] * inv_freq[None, :]
    angles = angles.reshape((angles.shape[0],) + (1,) * (values.ndim - 2) + (half_dim,))
    cosine = jnp.cos(angles)
    sine_part = jnp.sin(angles)
    first_half = values[..., :half_dim].astype(jnp.float32)
    second_half = values[..., half_dim:].astype(jnp.float32)
    return jnp.concatenate(
        [
            first_half * cosine - second_half * sine_part,
            second_half * cosine + first_half * sine_part,
        ],
        axis=-1,
    )


MESH = pl.DeviceIdType.MESH
VMEM = pltpu.VMEM


def greet(n_ep, n_tp):
    me = lax.axis_index("ep")
    t = lax.axis_index("tp")
    low, high = lax.rem(t, 2), lax.div(t, 2)
    n_high = n_tp // 2
    barrier = pltpu.get_barrier_semaphore()
    for k in range(1, n_ep):
        pl.semaphore_signal(
            barrier, inc=1, device_id={"ep": lax.rem(me + k, n_ep)}, device_id_type=MESH
        )
    for j in range(1, n_high):
        pl.semaphore_signal(
            barrier,
            inc=1,
            device_id={"tp": lax.rem(high + j, n_high) * 2 + low},
            device_id_type=MESH,
        )
    pl.semaphore_signal(barrier, inc=1, device_id={"tp": high * 2 + 1 - low}, device_id_type=MESH)
    pl.semaphore_wait(barrier, n_ep - 1 + n_high - 1 + 1)
    return me, t, low, high, n_high


def exchange_kernel(n_ep, n_tp, *refs):
    send_ref, kv_ref, out_ref, kvo_ref = refs[:4]
    own_sem, s1, r1, s2, r2, s3, r3 = refs[4:]
    me, t, low, high, n_high = greet(n_ep, n_tp)
    width = send_ref.shape[-1]

    def spot(kind, source, part):
        if kind == 0:
            start = pl.multiple_of(part * width, width)
            return out_ref.at[source, :, pl.ds(start, width)]
        return kvo_ref.at[source, part]

    def remote(src, dst, ssem, rsem, device):
        return pltpu.make_async_remote_copy(
            src_ref=src, dst_ref=dst, send_sem=ssem, recv_sem=rsem,
            device_id=device, device_id_type=MESH,
        )

    pending = []
    first = {}
    for kind in range(2):
        for k in range(1, n_ep):
            to = lax.rem(me + k, n_ep)
            src = send_ref.at[to] if kind == 0 else kv_ref
            copy = remote(src, spot(kind, me, t), s1.at[kind, k], r1.at[kind, k], {"ep": to})
            copy.start()
            first[kind, k] = copy
            pending.append(copy)
    local = []
    for kind in range(2):
        src = send_ref.at[me] if kind == 0 else kv_ref
        copy = pltpu.make_async_copy(src, spot(kind, me, t), own_sem.at[kind])
        copy.start()
        local.append(copy)
    partner = {"tp": high * 2 + 1 - low}
    second = {}

    def pass_on(kind, k):
        source = lax.rem(me - k + n_ep, n_ep)
        for j in range(1, n_high):
            from_high = lax.rem(high - j + n_high, n_high)
            second[kind, k, j].wait_recv()
            place = spot(kind, source, from_high * 2 + low)
            copy = remote(place, place, s3.at[kind, k, j], r3.at[kind, k, j], partner)
            copy.start()
            pending.append(copy)
            last.append(copy)

    last = []
    steps = [(kind, k) for kind in range(2) for k in range(n_ep)]
    for index, (kind, k) in enumerate(steps):
        source = lax.rem(me - k + n_ep, n_ep)
        if k == 0:
            local[kind].wait()
        else:
            first[kind, k].wait_recv()
        place = spot(kind, source, t)
        for j in range(1, n_high):
            to_high = lax.rem(high + j, n_high)
            copy = remote(
                place, place, s2.at[kind, k, j], r2.at[kind, k, j], {"tp": to_high * 2 + low}
            )
            copy.start()
            second[kind, k, j] = copy
            pending.append(copy)
        copy = remote(place, place, s3.at[kind, k, 0], r3.at[kind, k, 0], partner)
        copy.start()
        pending.append(copy)
        last.append(copy)
        if index >= 2:
            pass_on(*steps[index - 2])
    for step in steps[-2:]:
        pass_on(*step)
    for copy in last:
        copy.wait_recv()
    for copy in pending:
        copy.wait_send()


def exchange(send_rows, kv_pack, n_ep, n_tp):
    slots, width = send_rows.shape[1:]
    n_high = n_tp // 2
    sem = pltpu.SemaphoreType.DMA
    return pl.pallas_call(
        functools.partial(exchange_kernel, n_ep, n_tp),
        out_shape=(
            jax.ShapeDtypeStruct((n_ep, slots, n_tp * width), send_rows.dtype),
            jax.ShapeDtypeStruct((n_ep, n_tp) + kv_pack.shape, kv_pack.dtype),
        ),
        in_specs=[pl.BlockSpec(memory_space=VMEM)] * 2,
        out_specs=(pl.BlockSpec(memory_space=VMEM),) * 2,
        scratch_shapes=[
            sem((2,)),
            sem((2, n_ep)), sem((2, n_ep)),
            sem((2, n_ep, n_high)), sem((2, n_ep, n_high)),
            sem((2, n_ep, n_high)), sem((2, n_ep, n_high)),
        ],
        compiler_params=pltpu.CompilerParams(collective_id=0, has_side_effects=True),
        name="exchange",
    )(send_rows, kv_pack)


def give_back_kernel(n_ep, n_tp, *refs):
    part_ref, mix_ref, ret_ref, mixed_ref = refs[:4]
    low_in, high_out, high_in, final, mlow_in, mhigh_out, mhigh_in = refs[4:11]
    sa, ra, sb, rb, sc, rc, own_sem = refs[11:]
    me, t, low, high, n_high = greet(n_ep, n_tp)
    width = ret_ref.shape[-1]
    rows = mixed_ref.shape[0]
    f32 = jnp.float32
    partner = {"tp": high * 2 + 1 - low}

    def remote(src, dst, ssem, rsem, device):
        return pltpu.make_async_remote_copy(
            src_ref=src, dst_ref=dst, send_sem=ssem, recv_sem=rsem,
            device_id=device, device_id_type=MESH,
        )

    def target(k):
        return lax.rem(me + k, n_ep)

    def piece(k, which):
        if k == n_ep:
            return mix_ref.at[pl.ds(pl.multiple_of(which * rows, rows), rows), :]
        start = pl.multiple_of(which * width, width)
        return part_ref.at[target(k), :, pl.ds(start, width)]

    pending = []
    order = [k for k in range(1, n_ep)] + [0, n_ep]
    stage_a, stage_b, stage_c = {}, {}, []
    for k in order:
        for j in range(n_high):
            which = lax.rem(high + j, n_high) * 2 + 1 - low
            dst = low_in.at[k, j] if k < n_ep else mlow_in.at[j]
            copy = remote(piece(k, which), dst, sa.at[k, j], ra.at[k, j], partner)
            copy.start()
            stage_a[k, j] = copy
            pending.append(copy)

    def to_high(k):
        for j in range(1, n_high):
            peer = lax.rem(high + j, n_high)
            stage_a[k, j].wait_recv()
            got = low_in.at[k, j] if k < n_ep else mlow_in.at[j]
            out = high_out.at[k, j] if k < n_ep else mhigh_out.at[j]
            mine = piece(k, peer * 2 + low)
            out[...] = (mine[...].astype(f32) + got[...].astype(f32)).astype(out.dtype)
            dst = high_in.at[k, j] if k < n_ep else mhigh_in.at[j]
            copy = remote(out, dst, sb.at[k, j], rb.at[k, j], {"tp": peer * 2 + low})
            copy.start()
            stage_b[k, j] = copy
            pending.append(copy)

    def finish(k):
        stage_a[k, 0].wait_recv()
        got = low_in.at[k, 0] if k < n_ep else mlow_in.at[0]
        total = piece(k, t)[...].astype(f32) + got[...].astype(f32)
        for j in range(1, n_high):
            stage_b[k, j].wait_recv()
            arrived = high_in.at[k, j] if k < n_ep else mhigh_in.at[j]
            total = total + arrived[...].astype(f32)
        if k == n_ep:
            mixed_ref[...] = total.astype(mixed_ref.dtype)
            return
        if k == 0:
            ret_ref[me] = total.astype(ret_ref.dtype)
            return
        final[k] = total.astype(final.dtype)
        copy = remote(final.at[k], ret_ref.at[me], sc.at[k], rc.at[k], {"ep": target(k)})
        copy.start()
        stage_c.append(copy)
        pending.append(copy)

    for k in order:
        to_high(k)
    for k in order:
        finish(k)
    for copy in stage_c:
        copy.wait_recv()
    for copy in pending:
        copy.wait_send()


def give_back(partial, mix_part, n_ep, n_tp):
    slots, wide = partial.shape[1:]
    width, rows = wide // n_tp, mix_part.shape[0] // n_tp
    n_high = n_tp // 2
    sem = pltpu.SemaphoreType.DMA
    kind = partial.dtype
    return pl.pallas_call(
        functools.partial(give_back_kernel, n_ep, n_tp),
        out_shape=(
            jax.ShapeDtypeStruct((n_ep, slots, width), kind),
            jax.ShapeDtypeStruct((rows, mix_part.shape[1]), kind),
        ),
        in_specs=[pl.BlockSpec(memory_space=VMEM)] * 2,
        out_specs=(pl.BlockSpec(memory_space=VMEM),) * 2,
        scratch_shapes=[
            VMEM((n_ep, n_high, slots, width), kind),
            VMEM((n_ep, n_high, slots, width), kind),
            VMEM((n_ep, n_high, slots, width), kind),
            VMEM((n_ep, slots, width), kind),
            VMEM((n_high, rows, mix_part.shape[1]), kind),
            VMEM((n_high, rows, mix_part.shape[1]), kind),
            VMEM((n_high, rows, mix_part.shape[1]), kind),
            sem((n_ep + 1, n_high)), sem((n_ep + 1, n_high)),
            sem((n_ep + 1, n_high)), sem((n_ep + 1, n_high)),
            sem((n_ep,)), sem((n_ep,)), sem((1,)),
        ],
        compiler_params=pltpu.CompilerParams(collective_id=1, has_side_effects=True),
        name="give_back",
    )(partial, mix_part)


def attend_kernel(scale, heads, nope, bounds_ref, q_ref, kv_ref, wk_ref, wv_ref, place_ref, mix_ref, out_ref):
    lat = wk_ref.shape[0]
    n_tp = kv_ref.shape[1]
    queries = q_ref.shape[-1]
    block = queries
    own = block // n_tp
    vdim = wv_ref.shape[0] // heads
    f32, bf16 = jnp.float32, jnp.bfloat16
    factor = scale * math.log2(math.e)

    def step(index, state, masked):
        latents = kv_ref[index, :, :own, :].reshape(block, lat)
        rope_rows = jnp.concatenate(
            [kv_ref[index, part, own:, :] for part in range(n_tp)], axis=1
        )
        rot = lax.dot_general(
            rope_rows, place_ref[...], (((0,), (0,)), ((), ())), preferred_element_type=f32
        )
        values = lax.dot_general(
            wv_ref[...], latents, (((1,), (1,)), ((), ())), preferred_element_type=f32
        ).astype(bf16)
        result = []
        for h in range(heads):
            top, total, weighted = state[h]
            keys = (
                jnp.dot(latents, wk_ref[:, h * lat:(h + 1) * lat], preferred_element_type=f32) + rot
            ).astype(bf16)
            scores = jnp.dot(keys, q_ref[h], preferred_element_type=f32)
            if masked:
                key_id = lax.broadcasted_iota(jnp.int32, scores.shape, 0)
                query_id = lax.broadcasted_iota(jnp.int32, scores.shape, 1)
                scores = jnp.where(key_id <= query_id, scores, neg_big)
            new_top = jnp.maximum(top, jnp.max(scores, axis=0, keepdims=True))
            probs = jnp.exp2((scores - new_top) * factor)
            shrink = jnp.exp2((top - new_top) * factor)
            total = total * shrink + jnp.sum(probs, axis=0, keepdims=True)
            weighted = weighted * shrink + jnp.dot(
                values[h * vdim:(h + 1) * vdim], probs.astype(bf16), preferred_element_type=f32
            )
            result.append((new_top, total, weighted))
        return tuple(result)

    state = tuple(
        (
            jnp.full((1, queries), neg_big, f32),
            jnp.zeros((1, queries), f32),
            jnp.zeros((vdim, queries), f32),
        )
        for _ in range(heads)
    )
    state = lax.fori_loop(
        bounds_ref[0], bounds_ref[1], lambda i, run: step(i, run, False), state
    )
    state = step(bounds_ref[1], state, True)
    attn = jnp.concatenate([weighted / total for _, total, weighted in state], axis=0)
    attn = attn.T.astype(bf16)
    out_ref[...] = jnp.dot(attn, mix_ref[...], preferred_element_type=f32).astype(out_ref.dtype)


def attend(bounds, q_rows, kv_all, key_up, value_up, place, mix, scale, heads, nope):
    queries = q_rows.shape[-1]
    return pl.pallas_call(
        functools.partial(attend_kernel, scale, heads, nope),
        out_shape=jax.ShapeDtypeStruct((queries, mix.shape[1]), jnp.bfloat16),
        in_specs=[pl.BlockSpec(memory_space=pltpu.SMEM)] + [pl.BlockSpec(memory_space=VMEM)] * 6,
        out_specs=pl.BlockSpec(memory_space=VMEM),
        name="attend",
    )(bounds, q_rows, kv_all, key_up, value_up, place, mix)


def shards(
    queries,
    kv_latent,
    rope_key,
    kv_gain,
    kv_up,
    mix_out,
    moe_in,
    moe_gain,
    routes,
    route_weights,
    gate_w,
    up_w,
    down_w,
):
    n_ep, n_tp = lax.axis_size("ep"), lax.axis_size("tp")
    f32, bf16 = jnp.float32, jnp.bfloat16
    block_rows, heads_here, head_dim = queries.shape
    lat = kv_latent.shape[1]
    rope_dim = rope_key.shape[1]
    seq_len = block_rows * n_ep // SEQS
    ep_index = lax.axis_index("ep")
    query_start = ep_index * block_rows

    rows_here = routes.shape[0]
    top_count = routes.shape[1]
    experts = gate_w.shape[0] * n_ep
    mean_slots = top_count * rows_here // experts
    capacity = mean_slots + max(mean_slots // 16, 1)
    count = rows_here * top_count
    chosen = routes.T.reshape(-1)
    onehot = chosen[:, None] == jnp.arange(experts, dtype=jnp.int32)[None, :]
    entry = jnp.arange(count, dtype=jnp.int32)
    earlier = (entry[None, :] < entry[:, None]).astype(bf16)
    before = jnp.dot(earlier, onehot.astype(bf16), preferred_element_type=f32)
    slot_rank = jnp.sum(jnp.where(onehot, before, 0.0), axis=1).astype(jnp.int32)
    slot_dest = (chosen * capacity + slot_rank).reshape(top_count, rows_here)
    slot_ids = (
        jnp.arange(experts, dtype=jnp.int32)[:, None] * capacity
        + jnp.arange(capacity, dtype=jnp.int32)[None, :]
    )
    pick = slot_ids[:, :, None] == slot_dest[0][None, None, :]
    for choice in range(1, top_count):
        pick = pick | (slot_ids[:, :, None] == slot_dest[choice][None, None, :])
    send_rows = jnp.einsum(
        "scr,rd->scd", pick.astype(bf16), moe_in, preferred_element_type=f32
    ).astype(bf16)

    own_rows = kv_latent.shape[0]
    own_start = query_start + lax.axis_index("tp") * own_rows
    own_ids = own_start + jnp.arange(own_rows, dtype=jnp.int32)
    latent_rows = kv_latent.astype(f32)
    normed = (
        latent_rows
        * lax.rsqrt(jnp.mean(latent_rows * latent_rows, axis=-1, keepdims=True) + eps)
        * kv_gain
    ).astype(bf16)
    key_rot = rotate(rope_key, own_ids % seq_len).astype(bf16)
    kv_pack = jnp.concatenate([normed, key_rot.T], axis=0)

    arrived, kv_all = exchange(send_rows, kv_pack, n_ep, n_tp)

    query_index = query_start + jnp.arange(block_rows, dtype=jnp.int32)
    query_rot = rotate(queries[..., NOPE:], query_index % seq_len).astype(bf16)
    q_rows = jnp.concatenate([queries[..., :NOPE], query_rot], axis=-1).transpose(1, 2, 0)
    q_rows = jnp.pad(q_rows, ((0, 0), (0, lat - head_dim), (0, 0)))
    key_up = jnp.pad(kv_up[..., :NOPE], ((0, 0), (0, 0), (0, lat - NOPE))).reshape(lat, -1)
    value_up = kv_up[..., NOPE:].transpose(1, 2, 0).reshape(-1, lat)
    place = jnp.eye(rope_dim, lat, k=NOPE, dtype=bf16)
    bounds = jnp.stack([query_start // seq_len * seq_len // block_rows, ep_index]).astype(jnp.int32)
    mix_part = attend(
        bounds, q_rows, kv_all, key_up, value_up, place,
        mix_out.reshape(-1, mix_out.shape[-1]), 1.0 / math.sqrt(head_dim), heads_here, NOPE,
    )

    piece_f = arrived.astype(f32)
    scaled = (piece_f * moe_gain).astype(bf16)
    gate_acc = jnp.einsum("scd,df->scf", scaled, gate_w[0], preferred_element_type=f32)
    up_acc = jnp.einsum("scd,df->scf", scaled, up_w[0], preferred_element_type=f32)
    squares = jnp.sum(piece_f * piece_f, axis=-1)
    row_scale = lax.rsqrt(squares / D + eps)[..., None]
    hidden = (jax.nn.silu(gate_acc * row_scale) * (up_acc * row_scale)).astype(bf16)
    partial_value = jnp.einsum(
        "scf,fd->scd", hidden, down_w[0], preferred_element_type=f32
    ).astype(bf16)

    returned, mixed = give_back(partial_value, mix_part, n_ep, n_tp)
    moe_out = 0.0
    for choice in range(top_count):
        find = slot_dest[choice][:, None, None] == slot_ids[None]
        picked = jnp.einsum("rsc,scd->rd", find.astype(bf16), returned, preferred_element_type=f32)
        moe_out = moe_out + picked * route_weights[:, choice:choice + 1]
    return (mixed, moe_out.astype(bf16))


def solution(mesh):
    in_specs = (
        P("ep", "tp", None),
        P(("ep", "tp"), None),
        P(("ep", "tp"), None),
        P(),
        P(None, "tp", None),
        P("tp", None, None),
        P("ep", "tp"),
        P(),
        P("ep", None),
        P("ep", None),
        P("ep", None, "tp"),
        P("ep", None, "tp"),
        P("ep", "tp", None),
    )
    out_specs = (P(("ep", "tp"), None), P("ep", "tp"))
    return jax.shard_map(shards, mesh=mesh, in_specs=in_specs, out_specs=out_specs, check_vma=False)
```
